32 devices in a mesh: grp: 2 (over y), sp: 4 (over z), tp: 4 (over x, core).
Axes of the slice: x: 2, y: 2, z: 4, core: 2. Of those that a mesh axis runs over, the one named last changes fastest.
Arguments:
- queries: bfloat16 [8192, 1024], P(('grp', 'sp'), 'tp'), parts along dimension 0, may hold values from -6 to 6
- keys: bfloat16 [8192, 256], P(('grp', 'sp')), parts along dimension 0, may hold values from -6 to 6
- values: bfloat16 [8192, 256], P(('grp', 'sp')), parts along dimension 0, may hold values from -6 to 6
- query_gain: float32 [128], replicated, may hold values from 1.2 to 6, as said below
- key_gain: float32 [128], replicated, may hold values from 1.2 to 6, as said below
- out_weight: bfloat16 [1024, 2048], replicated, may hold values from -6 to 6
- residual_in: bfloat16 [8192, 2048], P(('grp', 'sp', 'tp')), parts along dimension 0, may hold values from -6 to 6
- norm_gain: float32 [2048], replicated, may hold values from 0.1 to 1.9
- gate_weight: bfloat16 [2048, 2816], P('sp', 'tp'), may hold values from -0.125 to 0.125
- up_weight: bfloat16 [2048, 2816], P('sp', 'tp'), may hold values from -0.125 to 0.125
- down_weight: bfloat16 [2816, 2048], P('tp', 'sp'), may hold values from -0.109375 to 0.109375
Outputs:
- layer_out: bfloat16 [8192, 2048], P(('grp', 'sp', 'tp')), parts along dimension 0
The draws below stay inside these ranges and needn't reach their ends.
There are 2 independent parts, one for each index of `grp`. The reference program is written for one: setup_inputs(seed, part) draws one part's arguments, and reference() takes and returns one part's arrays. A program takes and returns all parts, laid end to end along the dimension named above; an argument that names none is the same for every part. Nothing has to cross between parts.
Inputs may be any that keep to these rules, and one draw needn't show every extreme that they name: `query_gain`: positive gains. `key_gain`: positive gains.
All inputs are finite; a program needn't handle non-finite values.
Results may differ from the reference program's by a relative error of at most 0.015.
The reference program's roundings to bfloat16 on the way (of `query_rot`, `key_rot`, `probs`, `attended`, `normed` and `hidden`) count: a program that leaves them out, or rounds other values in their place, can miss the bound.
Values may be sent and summed in bfloat16 or wider, within the bound.
No kernel may reach another device: no remote copies, remote signals or barrier semaphores. Data moves between devices by JAX's collectives and lax.ppermute only.
A program may use at most 128 MiB of HBM per device.

```python
import jax
import jax.numpy as jnp
from jax import lax

D = 2048
HQ = 8
KV = 2
HD = 128
FF = 2816
GRID_W = 64
TOK_DEV = 1024
TOKENS = 4096


def shared_draw(key):
    key_rows = jax.random.truncated_normal(jax.random.fold_in(key, 1), -6.0, 6.0, (TOKENS, KV * HD), jnp.float32)
    query_rows = jax.random.truncated_normal(jax.random.fold_in(key, 2), -6.0, 6.0, (TOKENS, HQ * HD), jnp.float32)
    return (query_rows, key_rows)


def draw_queries(key, part):
    return shared_draw(key)[0].astype(jnp.bfloat16)


def draw_keys(key, part):
    return shared_draw(key)[1].astype(jnp.bfloat16)


def draw_query_gain(key, part):
    return jax.random.uniform(jax.random.fold_in(key, 11), (HD,), jnp.float32, 1.2, 1.7)


def draw_key_gain(key, part):
    return jax.random.uniform(jax.random.fold_in(key, 12), (HD,), jnp.float32, 1.2, 1.7)


def block_levels(own_key, extent, pieces, low, largest):
    level = 1.0
    for dim, parts in pieces:
        draws = jax.random.uniform(jax.random.fold_in(jax.random.fold_in(own_key, 6), dim), (parts,), jnp.float32, low / len(pieces), largest / len(pieces))
        level = level * jnp.repeat(jnp.exp(draws), extent[dim] // parts).reshape((-1,) + (1,) * (len(extent) - 1 - dim))
    return level


def centred(own_key, extent, deviation, bound, shards=(), kind=jnp.bfloat16):
    result = jax.random.normal(own_key, extent, jnp.float32) * deviation
    if len(shards) > 0:
        result = block_levels(own_key, extent, shards, -0.22, 0.18) * result
    return jnp.clip(result, min=-bound, max=bound).astype(kind)


def setup_inputs(seed: int = 0, part: int = 0) -> dict:
    arg_keys = jax.random.split(jax.random.key(seed), 12)
    part_keys = jax.random.split(jax.random.fold_in(arg_keys[11], part), 12)
    queries = draw_queries(jax.random.fold_in(jax.random.fold_in(arg_keys[11], part), 71), part)
    keys = draw_keys(jax.random.fold_in(jax.random.fold_in(arg_keys[11], part), 71), part)
    values = centred(part_keys[2], (TOKENS, KV * HD), 1.0, 6.0, ((0, 4),))
    query_gain = draw_query_gain(jax.random.fold_in(arg_keys[11], 71), part)
    key_gain = draw_key_gain(jax.random.fold_in(arg_keys[11], 71), part)
    out_weight = centred(arg_keys[5], (HQ * HD, D), 0.4, 6.0)
    residual_in = centred(part_keys[6], (TOKENS, D), 1.0, 6.0, ((0, 16),))
    norm_gain = jnp.clip(1.0 + 0.18 * jax.random.normal(arg_keys[7], (D,), jnp.float32), 0.1, 1.9)
    gate_weight = centred(arg_keys[8], (D, FF), D ** -0.5, 0.125, ((0, 4), (1, 4)))
    up_weight = centred(arg_keys[9], (D, FF), D ** -0.5, 0.125, ((0, 4), (1, 4)))
    down_weight = centred(arg_keys[10], (FF, D), FF ** -0.5, 0.109375, ((0, 4), (1, 4)))
    return {"queries": queries, "keys": keys, "values": values, "query_gain": query_gain, "key_gain": key_gain, "out_weight": out_weight, "residual_in": residual_in, "norm_gain": norm_gain, "gate_weight": gate_weight, "up_weight": up_weight, "down_weight": down_weight}


def rotate(widened, positions):
    half = HD // 2
    inverse = 10000.0 ** (-jnp.arange(0, half, 2, dtype=jnp.float32) / half)
    grid_row = (positions // GRID_W).astype(jnp.float32)
    grid_col = (positions % GRID_W).astype(jnp.float32)
    angles = jnp.concatenate([grid_row[:, None] * inverse[None], grid_col[:, None] * inverse[None]], axis=-1)
    cosine = jnp.cos(angles)[:, None, :]
    sine = jnp.sin(angles)[:, None, :]
    pairs = widened.reshape(widened.shape[0], widened.shape[1], half, 2)
    first = pairs[..., 0]
    second = pairs[..., 1]
    turned = jnp.stack([first * cosine - second * sine, first * sine + second * cosine], axis=-1)
    return turned.reshape(widened.shape)

def prepare(source, gain, positions, heads):
    widened = source.astype(jnp.float32).reshape(source.shape[0], heads, HD)
    widened = widened * lax.rsqrt(lax.optimization_barrier(jnp.mean(widened * widened, axis=-1, keepdims=True)) + 1e-06) * gain
    return rotate(widened, positions).astype(jnp.bfloat16)

def reference(queries, keys, values, query_gain, key_gain, out_weight, residual_in, norm_gain, gate_weight, up_weight, down_weight):
    positions = jnp.arange(TOKENS, dtype=jnp.int32)
    query_rot = prepare(queries, query_gain, positions, HQ).transpose(1, 0, 2)
    key_rot = prepare(keys, key_gain, positions, KV).transpose(1, 0, 2)
    value_heads = values.reshape(TOKENS, KV, HD).transpose(1, 0, 2)
    group = HQ // KV
    scale = HD ** (-0.5)

    def one_head(head):
        key_block = key_rot[head // group]
        value_block = value_heads[head // group]
        query_blocks = query_rot[head].reshape(TOKENS // TOK_DEV, TOK_DEV, HD)

        def one_block(query_block):
            scores = jnp.dot(query_block, key_block.T, preferred_element_type=jnp.float32) * scale
            peak = lax.optimization_barrier(jnp.max(scores, axis=1, keepdims=True))
            raised = jnp.exp(scores - peak)
            denominator = lax.optimization_barrier(jnp.sum(raised, axis=1, keepdims=True))
            probs = raised.astype(jnp.bfloat16)
            mixed = jnp.dot(probs, value_block, preferred_element_type=jnp.float32)
            return (mixed / denominator).astype(jnp.bfloat16)
        return lax.map(one_block, query_blocks).reshape(TOKENS, HD)
    attended = lax.map(one_head, jnp.arange(HQ, dtype=jnp.int32))
    attended = attended.transpose(1, 0, 2).reshape(TOKENS, HQ * HD)
    middle = residual_in.astype(jnp.float32) + jnp.dot(attended, out_weight, preferred_element_type=jnp.float32)
    normed = middle * lax.rsqrt(lax.optimization_barrier(jnp.mean(middle * middle, axis=-1, keepdims=True)) + 1e-06) * norm_gain
    normed = normed.astype(jnp.bfloat16)
    gate_act = jnp.dot(normed, gate_weight, preferred_element_type=jnp.float32)
    up_act = jnp.dot(normed, up_weight, preferred_element_type=jnp.float32)
    hidden = (jax.nn.silu(gate_act) * up_act).astype(jnp.bfloat16)
    mixer_out = jnp.dot(hidden, down_weight, preferred_element_type=jnp.float32)
    return (middle + mixer_out).astype(jnp.bfloat16)
```

```python
import functools

import jax
import jax.numpy as jnp
from jax import lax
from jax.experimental import pallas as pl
from jax.experimental.pallas import tpu as pltpu
from jax.sharding import PartitionSpec as P

HQ = 8
KV = 2
HD = 128
GRID_W = 64
LOG2E = 1.4426950408889634
AXES = ("grp", "sp", "tp")
BF = jnp.bfloat16
F32 = jnp.float32


def params(limit=56 << 20):
    return pltpu.CompilerParams(vmem_limit_bytes=limit)


def turn(v, cos_sin, gain, grid_rows):
    v = v * lax.rsqrt(jnp.mean(v * v, axis=-1, keepdims=True) + 1e-06) * gain
    lane = lax.broadcasted_iota(jnp.int32, v.shape, 1)
    swapped = jnp.where(lane % 2 == 0, pltpu.roll(v, HD - 1, 1), pltpu.roll(v, 1, 1))
    rows = v.shape[0] // GRID_W
    lane3 = lax.broadcasted_iota(jnp.int32, (rows, GRID_W, HD), 2)

    def table(c):
        row_part = grid_rows(c)[:, None, :]
        col_part = cos_sin[c, -GRID_W:, :][None]
        return jnp.where(lane3 < HD // 2, row_part, col_part).reshape(v.shape)

    return (v * table(0) + swapped * table(1)).astype(BF)


def prep_kv(keys, values, tables, gain, kv_head, half, halves):
    rows = keys.shape[0] // halves
    grid_rows = rows // GRID_W

    def body(s_ref, k_ref, v_ref, t_ref, g_ref, o_ref):
        def pick(c):
            return t_ref[c, pl.ds(pl.multiple_of(s_ref[1] * grid_rows, grid_rows), grid_rows), :]

        o_ref[:, :HD] = turn(k_ref[...].astype(F32), t_ref, g_ref[...], pick)
        o_ref[:, HD:] = v_ref[...]

    block = pl.BlockSpec((rows, HD), lambda i, s: (s[1], s[0]))
    return pl.pallas_call(
        body,
        grid_spec=pltpu.PrefetchScalarGridSpec(
            num_scalar_prefetch=1,
            grid=(1,),
            in_specs=[
                block,
                block,
                pl.BlockSpec(tables.shape, lambda i, s: (0, 0, 0)),
                pl.BlockSpec((1, HD), lambda i, s: (0, 0)),
            ],
            out_specs=pl.BlockSpec((rows, 2 * HD), lambda i, s: (0, 0)),
        ),
        out_shape=jax.ShapeDtypeStruct((rows, 2 * HD), BF),
        compiler_params=params(),
        name="prep_kv",
    )(jnp.stack([kv_head, half]).astype(jnp.int32), keys, values, tables, gain.reshape(1, HD))


def prep_q(queries, tables, gain):
    rows = queries.shape[0]
    tile = 256
    heads = queries.shape[1] // HD
    grid_rows = tile // GRID_W

    def body(q_ref, t_ref, g_ref, o_ref):
        i = pl.program_id(0)

        def pick(c):
            return t_ref[c, pl.ds(i * grid_rows, grid_rows), :]

        for h in range(heads):
            cols = slice(h * HD, (h + 1) * HD)
            o_ref[:, cols] = turn(q_ref[:, cols].astype(F32), t_ref, g_ref[...], pick)

    return pl.pallas_call(
        body,
        grid=(rows // tile,),
        in_specs=[
            pl.BlockSpec((tile, heads * HD), lambda i: (i, 0)),
            pl.BlockSpec(tables.shape, lambda i: (0, 0, 0)),
            pl.BlockSpec((1, HD), lambda i: (0, 0)),
        ],
        out_specs=pl.BlockSpec((tile, heads * HD), lambda i: (i, 0)),
        out_shape=jax.ShapeDtypeStruct(queries.shape, BF),
        compiler_params=params(),
        name="prep_q",
    )(queries, tables, gain.reshape(1, HD))


def attention(query_rot, blocks):
    rows, width = query_rot.shape
    heads = width // HD
    count = len(blocks)
    size = blocks[0].shape[0]
    tile = 512 if count * size <= 8192 else 128
    factor = HD ** (-0.5) * LOG2E

    def body(q_ref, *refs):
        kv = refs[:count]
        o_ref, s_ref = refs[count:]
        q = q_ref[...]
        peak = None
        for b in range(count):
            s = lax.dot_general(
                q, kv[b][:, :HD], (((1,), (1,)), ((), ())), preferred_element_type=F32
            )
            s_ref[b] = s
            top = jnp.max(s, axis=1, keepdims=True)
            peak = top if peak is None else jnp.maximum(peak, top)
        ones = jnp.ones((size, HD), BF)
        total = jnp.zeros((tile, 2 * HD), F32)
        for b in range(count):
            p = jnp.exp2((s_ref[b] - peak) * factor).astype(BF)
            v = jnp.concatenate([kv[b][:, HD:], ones], axis=1)
            total += jnp.dot(p, v, preferred_element_type=F32)
        o_ref[...] = (total[:, :HD] / total[:, HD:]).astype(BF)

    spec = pl.BlockSpec((tile, HD), lambda h, i: (i, h))
    return pl.pallas_call(
        body,
        grid=(heads, rows // tile),
        in_specs=[spec] + [pl.BlockSpec((size, 2 * HD), lambda h, i: (0, 0))] * count,
        out_specs=spec,
        out_shape=jax.ShapeDtypeStruct((rows, width), BF),
        scratch_shapes=[pltpu.VMEM((count, tile, size), F32)],
        compiler_params=params(),
        name="attention",
    )(query_rot, *blocks)


def project(attended, residual, out_weight, norm_gain, place, nblk):
    slots = len(attended)
    rows, cols = attended[0].shape
    own, width = residual[0].shape
    blk = width // nblk

    def body(t_ref, *refs):
        att = refs[:slots]
        res = refs[slots : 2 * slots]
        w_ref, g_ref, x_ref, m_ref = refs[2 * slots :]
        for r in range(slots):
            start = pl.multiple_of((t_ref[0] ^ r) * own, own)
            acc = res[r][...].astype(F32)
            for s in range(slots):
                w_start = pl.multiple_of((t_ref[0] ^ s) * cols, cols)
                acc += jnp.dot(
                    att[s][pl.ds(start, own), :],
                    w_ref[pl.ds(w_start, cols), :],
                    preferred_element_type=F32,
                )
            if r == 0:
                m_ref[...] = acc
            x = acc * lax.rsqrt(jnp.mean(acc * acc, axis=-1, keepdims=True) + 1e-06) * g_ref[...]
            x = x.astype(BF)
            for n in range(nblk):
                x_ref[n, pl.ds(start, own), :] = x[:, n * blk : (n + 1) * blk]

    vm = pl.BlockSpec(memory_space=pltpu.VMEM)
    return pl.pallas_call(
        body,
        in_specs=[pl.BlockSpec(memory_space=pltpu.SMEM)] + [vm] * (2 * slots + 2),
        out_specs=[vm, vm],
        out_shape=[
            jax.ShapeDtypeStruct((nblk, rows, blk), BF),
            jax.ShapeDtypeStruct((own, width), F32),
        ],
        compiler_params=params(),
        name="project",
    )(place.reshape(1), *attended, *residual, out_weight, norm_gain.reshape(1, width))


def gate_up(x, weights, index):
    nblk, rows, blk = x.shape
    count = len(weights)
    both = weights[0].shape[1]
    ff = both // 2
    tile = 256

    def body(i_ref, x_ref, *refs):
        ws = refs[:count]
        o_ref = refs[count]
        acc = jnp.zeros((tile, both), F32)
        for n in range(count):
            acc += jnp.dot(x_ref[i_ref[n]], ws[n][...], preferred_element_type=F32)
        gate = acc[:, :ff]
        o_ref[...] = (gate / (1.0 + jnp.exp(-gate)) * acc[:, ff:]).astype(BF)

    return pl.pallas_call(
        body,
        grid_spec=pltpu.PrefetchScalarGridSpec(
            num_scalar_prefetch=1,
            grid=(rows // tile,),
            in_specs=[pl.BlockSpec((nblk, tile, blk), lambda i, s: (0, i, 0))]
            + [pl.BlockSpec((blk, both), lambda i, s: (0, 0))] * count,
            out_specs=pl.BlockSpec((tile, ff), lambda i, s: (i, 0)),
        ),
        out_shape=jax.ShapeDtypeStruct((rows, ff), BF),
        compiler_params=params(),
        name="gate_up",
    )(index, x, *weights)


def down(hidden, weight, place, slots):
    rows, ff = hidden.shape
    cols = weight.shape[1]
    own = rows // slots

    def body(t_ref, h_ref, w_ref, k_ref, s_ref):
        for s in range(slots):
            start = pl.multiple_of((t_ref[0] ^ s) * own, own)
            y = jnp.dot(h_ref[pl.ds(start, own), :], w_ref[...], preferred_element_type=F32)
            if s % 2:
                s_ref[s // 2] = y.astype(BF)
            else:
                k_ref[s // 2] = y.astype(BF)

    vm = pl.BlockSpec(memory_space=pltpu.VMEM)
    shape = jax.ShapeDtypeStruct((slots // 2, own, cols), BF)
    return pl.pallas_call(
        body,
        in_specs=[pl.BlockSpec(memory_space=pltpu.SMEM), vm, vm],
        out_specs=[vm, vm],
        out_shape=[shape, shape],
        compiler_params=params(),
        name="down",
    )(place.reshape(1), hidden, weight)


def finish(middle, parts, index, valid):
    rows, width = middle.shape
    flat = [a for part in parts for a in part]
    blk = parts[0][0].shape[1]

    def body(i_ref, v_ref, m_ref, *refs):
        o_ref = refs[-1]
        at = 0
        for n, part in enumerate(parts):
            mine = refs[at : at + len(part)]
            at += len(part)

            @pl.when(v_ref[n] == 1)
            def _():
                where = pl.ds(pl.multiple_of(i_ref[n] * blk, blk), blk)
                total = mine[0][...].astype(F32)
                for other in mine[1:]:
                    total += other[...].astype(F32)
                o_ref[:, where] = (m_ref[:, where] + total).astype(BF)

    vm = pl.BlockSpec(memory_space=pltpu.VMEM)
    sm = pl.BlockSpec(memory_space=pltpu.SMEM)
    return pl.pallas_call(
        body,
        in_specs=[sm, sm] + [vm] * (1 + len(flat)),
        out_specs=vm,
        out_shape=jax.ShapeDtypeStruct((rows, width), BF),
        compiler_params=params(),
        name="finish",
    )(index, valid, middle, *flat)


def solution(mesh):
    ngrp, nsp, ntp = (mesh.shape[a] for a in AXES)

    def move(a, target):
        pairs = []
        for g in range(ngrp):
            for z in range(nsp):
                for t in range(ntp):
                    to = target(g, z, t)
                    if to is not None:
                        pairs.append(
                            ((g * nsp + z) * ntp + t, (to[0] * nsp + to[1]) * ntp + to[2])
                        )
        return lax.ppermute(a, AXES, pairs)

    def gather_tp(a):
        got = {0: a}
        bit = ntp // 2
        while bit:
            for s in list(got):
                got[s | bit] = move(got[s], lambda g, z, t: (g, z, t ^ bit))
            bit //= 2
        return [got[s] for s in range(ntp)]

    def local(
        queries,
        keys,
        values,
        query_gain,
        key_gain,
        out_weight,
        residual_in,
        norm_gain,
        gate_weight,
        up_weight,
        down_weight,
    ):
        rows = queries.shape[0]
        heads_here = queries.shape[1] // HD
        g = lax.axis_index("grp")
        z = lax.axis_index("sp")
        t = lax.axis_index("tp")

        plane_rows = rows // GRID_W
        half = HD // 2
        inverse = 10000.0 ** (-jnp.arange(0, half, 2, dtype=F32) / half)
        inverse = jnp.tile(jnp.repeat(inverse, 2), 2)
        spots = jnp.concatenate(
            [z * plane_rows + jnp.arange(plane_rows), jnp.arange(GRID_W)]
        ).astype(F32)
        angles = spots[:, None] * inverse[None]
        sign = jnp.where(jnp.arange(HD) % 2 == 0, -1.0, 1.0).astype(F32)
        tables = jnp.stack([jnp.cos(angles), jnp.sin(angles) * sign])

        kv_head = t * heads_here // (HQ // KV)
        kv_own = prep_kv(keys, values, tables, key_gain, kv_head, t % 2, 2)
        kv_parts = [kv_own]
        for k in range(1, nsp):
            kv_parts.append(move(kv_own, lambda g, z, t: (g, (z + k) % nsp, t)))
        kv_parts += [move(a, lambda g, z, t: (g, z, t ^ 1)) for a in kv_parts]

        residual = gather_tp(residual_in)

        share = ngrp if (down_weight.shape[1] // ngrp) % 128 == 0 else 1
        both = jnp.concatenate([gate_weight, up_weight], axis=1)
        part = g % share

        def spread(full, dim):
            size = full.shape[dim] // share
            mine = lax.dynamic_slice_in_dim(full, part * size, size, dim)
            out = []
            direct = {}
            for k in range(1, nsp):
                direct[k] = move(
                    mine,
                    lambda g, z, t: (g, (z + k) % nsp, t)
                    if abs((z + k) % nsp - z) < nsp - 1
                    else None,
                )
            far = {}
            if nsp > 3:
                if nsp == 4:
                    far[0] = move(
                        direct[2], lambda g, z, t: {1: (g, 0, t), 2: (g, 3, t)}.get(z)
                    )
                else:
                    far[0] = move(direct[2], lambda g, z, t: (g, 0, t) if z == 1 else None)
                    far[1] = move(
                        direct[nsp - 2],
                        lambda g, z, t: (g, nsp - 1, t) if z == nsp - 2 else None,
                    )
            else:
                far[0] = move(
                    mine,
                    lambda g, z, t: (g, nsp - 1 - z, t) if z in (0, nsp - 1) else None,
                )
            for k in range(1, nsp):
                def ok(zz, k=k):
                    return abs((zz - k) % nsp - zz) < nsp - 1

                out.append((direct[k], (z - k) % nsp, ok))
            for f, a in far.items():
                if len(far) == 1:
                    out.append(
                        (a, jnp.where(z == 0, nsp - 1, 0), lambda zz: zz in (0, nsp - 1))
                    )
                elif f == 0:
                    out.append((a, jnp.int32(nsp - 1), lambda zz: zz == 0))
                else:
                    out.append((a, jnp.int32(0), lambda zz: zz == nsp - 1))
            result = []
            for s in range(share):
                at = (part + s) % share
                own = lax.dynamic_slice_in_dim(full, at * size, size, dim)
                result.append((own, z * share + at, lambda zz: True))
            for a, plane, ok in out:
                result.append((a, plane * share + part, ok))
                for s in range(1, share):
                    b = move(
                        a,
                        lambda g, z, t: (
                            g - g % share + (g + s) % share,
                            z,
                            t,
                        )
                        if ok(z)
                        else None,
                    )
                    result.append((b, plane * share + (part - s) % share, ok))
            return result

        up_parts = spread(both, 0)
        down_parts = spread(down_weight, 1)

        query_rot = prep_q(queries, tables, query_gain)
        attended = gather_tp(attention(query_rot, kv_parts))
        x, middle = project(attended, residual, out_weight, norm_gain, t, nsp * share)

        index = jnp.stack([i for _, i, _ in up_parts]).astype(jnp.int32)
        hidden = gate_up(x, [w for w, _, _ in up_parts], index)

        parts = []
        for w, _, ok in down_parts:
            keep, send = down(hidden, w, t, ntp)
            bit = 1
            while True:
                got = move(send, lambda g, z, t: (g, z, t ^ bit) if ok(z) else None)
                if keep.shape[0] == 1:
                    parts.append((keep[0], got[0]))
                    break
                total = (keep.astype(F32) + got.astype(F32)).astype(BF)
                keep, send = total[0::2], total[1::2]
                bit *= 2
        index = jnp.stack([i for _, i, _ in down_parts]).astype(jnp.int32)
        valid = jnp.stack(
            [
                jnp.array([int(ok(zz)) for zz in range(nsp)], jnp.int32)[z]
                for _, _, ok in down_parts
            ]
        )
        return finish(middle, parts, index, valid)

    placed = (
        P(("grp", "sp"), "tp"),
        P(("grp", "sp"), None),
        P(("grp", "sp"), None),
        P(),
        P(),
        P(),
        P(("grp", "sp", "tp"), None),
        P(),
        P("sp", "tp"),
        P("sp", "tp"),
        P("tp", "sp"),
    )
    return jax.shard_map(
        local, mesh=mesh, in_specs=placed, out_specs=P(("grp", "sp", "tp"), None), check_vma=False
    )
```
